32 devices in a mesh: grp: 2 (over y), sp: 4 (over z), tp: 4 (over x, core).
Axes of the slice: x: 2, y: 2, z: 4, core: 2. Of those that a mesh axis runs over, the one named last changes fastest.
Arguments:
- starting_stream: bfloat16 [3072, 2048], P(('grp', 'sp'), 'tp'), parts along dimension 0, may hold values from -45 to 45
- multiplier_matrix: bfloat16 [2, 2048, 2048], P(None, 'sp', 'tp'), may hold values from -0.125 to 0.125
- memory_path_matrix: bfloat16 [2, 2048, 2048], P(None, 'sp', 'tp'), may hold values from -0.125 to 0.125
- filter_coefficients: bfloat16 [2, 4, 2048], P(None, None, 'tp'), may hold values from -3 to 3
- memory_valve_matrix: bfloat16 [2, 8, 256, 256], P(None, 'tp'), may hold values from -0.375 to 0.375
- entry_valve_matrix: bfloat16 [2, 8, 256, 256], P(None, 'tp'), may hold values from -0.375 to 0.375
- forgetting_parameters: float32 [2, 2048], P(None, 'tp'), may hold values from 3 to 15
- timestep_forgetting_multiplier: float32 [3072], P(('grp', 'sp')), parts along dimension 0, may hold values from 0.5 to 2
- spike_extra: float32 [3072, 2048], P(('grp', 'sp'), 'tp'), parts along dimension 0, may hold values from -0.7 to 0
- exit_projector_matrix: bfloat16 [2, 2048, 2048], P(None, 'tp', 'sp'), may hold values from -0.125 to 0.125
- prelude_rms_gains: float32 [2, 2048], replicated, may hold values from 0.1 to 1.9
- finishing_rms_gains: float32 [2048], P('tp'), may hold values from 0.1 to 1.9
Outputs:
- result: bfloat16 [3072, 2048], P(('grp', 'sp'), 'tp'), parts along dimension 0
The draws below stay inside these ranges and needn't reach their ends.
There are 2 independent parts, one for each index of `grp`. The reference program is written for one: setup_inputs(seed, part) draws one part's arguments, and reference() takes and returns one part's arrays. A program takes and returns all parts, laid end to end along the dimension named above; an argument that names none is the same for every part. Nothing has to cross between parts.
All inputs are finite; a program needn't handle non-finite values.
Results may differ from the reference program's by a relative error of at most 0.015.
Values may be sent and summed in bfloat16 or wider, within the bound.
No kernel may reach another device: no remote copies, remote signals or barrier semaphores. Data moves between devices by JAX's collectives and lax.ppermute only.
A program may use at most 64 MiB of HBM per device.

```python
import math
import jax
import jax.numpy as jnp
from jax import lax

D = 2048
W = 2048
BLOCK_W = 256
BLOCKS = 8
CONV = 4
LAYERS = 2
TOK_DEV = 384
TOKENS = 1536
N_TP = 4


def draw_starting_stream(key, part):
    keys = jax.random.split(key, 3)
    columns = jnp.arange(D, dtype=jnp.float32)
    col_scale = jnp.exp(math.log(4.0) * columns / D) * jax.random.uniform(keys[1], (D,), jnp.float32, 0.7, 1.4)
    row_scale = jnp.exp(jax.random.uniform(keys[2], (TOKENS, 1), jnp.float32, math.log(0.5), math.log(2.0)))
    base = jnp.clip(jax.random.normal(keys[0], (TOKENS, D), jnp.float32), -4.0, 4.0)
    return (base * col_scale[None, :] * row_scale).astype(jnp.bfloat16)


def draw_forgetting_parameters(key, part):
    keys = jax.random.split(key, 3)
    share_fast = 0.5
    fast = jax.random.bernoulli(keys[0], share_fast, (LAYERS, W))
    fast_rate = jnp.exp(jax.random.uniform(keys[1], (LAYERS, W), jnp.float32, math.log(0.01), math.log(0.03)))
    slow_rate = jnp.exp(jax.random.uniform(keys[2], (LAYERS, W), jnp.float32, math.log(0.1), math.log(0.5))) / (4.0 * TOKENS)
    rate = jnp.where(fast, fast_rate, slow_rate)
    return -jnp.log(jnp.expm1(rate))


def draw_timestep_forgetting_multiplier(key, part):
    counted = TOKENS // TOK_DEV
    values = jnp.exp(jax.random.uniform(key, (counted,), jnp.float32, math.log(0.5), math.log(2.0)))
    return jnp.repeat(values, TOK_DEV, total_repeat_length=TOKENS)


def draw_spike_extra(key, part):
    keys = jax.random.split(key, 2)
    spots = jax.random.randint(keys[0], (4,), 0, TOKENS)
    places = jnp.arange(TOKENS, dtype=jnp.int32)
    struck = jnp.any(places[:, None] == spots[None, :], axis=1)
    depth = jnp.log(jax.random.uniform(keys[1], (TOKENS, W), jnp.float32, 0.5, 0.8))
    return jnp.where(struck[:, None], depth, 0.0)


def levels(own_key, dims, shards, least, high):
    factor_of, own = 1.0, jax.random.fold_in(own_key, 6)
    for axis_at, shards_of in shards:
        draws = jnp.exp(jax.random.uniform(jax.random.fold_in(own, axis_at), (shards_of,), jnp.float32, least / len(shards), high / len(shards)))
        factor_of = factor_of * jnp.repeat(draws, dims[axis_at] // shards_of).reshape([-1 if axis == axis_at else 1 for axis in range(len(dims))])
    return factor_of


def gaussian(stream_key, shape, scale, reach, shards=(), held_as=jnp.bfloat16):
    level = levels(stream_key, shape, shards, -0.22, 0.18) if shards else 1.0
    array = jax.random.normal(stream_key, shape, jnp.float32) * scale * level
    return jnp.minimum(jnp.maximum(array, -reach), reach).astype(held_as)


def setup_inputs(seed: int = 0, part: int = 0) -> dict:
    seeds = jax.random.split(jax.random.key(seed), 13)
    part_keys = jax.random.split(jax.random.fold_in(seeds[12], part), 13)
    return {
        "starting_stream": draw_starting_stream(jax.random.fold_in(jax.random.fold_in(seeds[12], part), 71), part),
        "multiplier_matrix": gaussian(seeds[1], (LAYERS, D, W), D ** -0.5, 0.125, ((1, 4), (2, 4))),
        "memory_path_matrix": gaussian(seeds[2], (LAYERS, D, W), D ** -0.5, 0.125, ((1, 4), (2, 4))),
        "filter_coefficients": gaussian(seeds[3], (LAYERS, CONV, W), CONV ** -0.5, 3.0, ((2, 4),)),
        "memory_valve_matrix": gaussian(seeds[4], (LAYERS, BLOCKS, BLOCK_W, BLOCK_W), BLOCK_W ** -0.5, 0.375, ((1, 4),)),
        "entry_valve_matrix": gaussian(seeds[5], (LAYERS, BLOCKS, BLOCK_W, BLOCK_W), BLOCK_W ** -0.5, 0.375, ((1, 4),)),
        "forgetting_parameters": draw_forgetting_parameters(jax.random.fold_in(seeds[12], 71), part),
        "timestep_forgetting_multiplier": draw_timestep_forgetting_multiplier(jax.random.fold_in(jax.random.fold_in(seeds[12], part), 71), part),
        "spike_extra": draw_spike_extra(jax.random.fold_in(jax.random.fold_in(seeds[12], part), 71), part),
        "exit_projector_matrix": gaussian(seeds[9], (LAYERS, W, D), W ** -0.5, 0.125, ((1, 4), (2, 4))),
        "prelude_rms_gains": jnp.clip(1.0 + 0.18 * jax.random.normal(seeds[10], (LAYERS, D), jnp.float32), 0.1, 1.9),
        "finishing_rms_gains": jnp.clip(1.0 + 0.18 * jax.random.normal(seeds[11], (D,), jnp.float32), 0.1, 1.9),
    }


EPSILON = 1e-06
SQUASH_POWER = 8.0

def norm_rows(values, gain):
    mean_square = lax.optimization_barrier(jnp.mean(values * values, axis=-1, keepdims=True))
    return values * lax.rsqrt(mean_square + EPSILON) * gain

def combine_pairs(earlier, later):
    return (earlier[0] * later[0], later[0] * earlier[1] + later[1])

def reference(starting_stream, multiplier_matrix, memory_path_matrix, filter_coefficients, memory_valve_matrix, entry_valve_matrix, forgetting_parameters, timestep_forgetting_multiplier, spike_extra, exit_projector_matrix, prelude_rms_gains, finishing_rms_gains):
    stream = starting_stream
    full_width = memory_path_matrix.shape[2]
    per_block = full_width // N_TP
    for tier_number in range(LAYERS):
        floats = stream.astype(jnp.float32)
        normed = norm_rows(floats, prelude_rms_gains[tier_number]).astype(jnp.bfloat16)
        branch = jnp.dot(normed, multiplier_matrix[tier_number], preferred_element_type=jnp.float32).astype(jnp.bfloat16)
        recurrent = jnp.dot(normed, memory_path_matrix[tier_number], preferred_element_type=jnp.float32).astype(jnp.bfloat16)
        padded = jnp.concatenate([jnp.zeros((CONV - 1, full_width), jnp.bfloat16), recurrent], axis=0)
        conv_sum = jnp.zeros((TOKENS, full_width), jnp.float32)
        for offset in range(CONV):
            conv_sum = conv_sum + padded[offset:offset + TOKENS].astype(jnp.float32) * filter_coefficients[tier_number, offset].astype(jnp.float32)
        convolved = conv_sum.astype(jnp.bfloat16)
        blocks = convolved.astype(jnp.float32).reshape(TOKENS, BLOCKS, BLOCK_W)
        memory_valve_amount = jax.nn.sigmoid(jnp.einsum('tnc,ncd->tnd', blocks, memory_valve_matrix[tier_number].astype(jnp.float32)).reshape(TOKENS, full_width))
        inject = jax.nn.sigmoid(jnp.einsum('tnc,ncd->tnd', blocks, entry_valve_matrix[tier_number].astype(jnp.float32)).reshape(TOKENS, full_width))
        logarithmic_persistence = -SQUASH_POWER * memory_valve_amount * jax.nn.softplus(-forgetting_parameters[tier_number])[None, :] * timestep_forgetting_multiplier[:, None] + spike_extra
        keep_rate = jnp.exp(logarithmic_persistence)
        driven = inject * convolved.astype(jnp.float32) * jnp.sqrt(-jnp.expm1(2.0 * logarithmic_persistence))
        state_seq = lax.associative_scan(combine_pairs, (keep_rate, driven), axis=0)[1]
        mixed_in = (jax.nn.gelu(branch.astype(jnp.float32)) * state_seq).astype(jnp.bfloat16)
        mixed_sum = jnp.zeros((TOKENS, D), jnp.float32)
        for block_no in range(N_TP):
            lower = block_no * per_block
            product = jnp.dot(mixed_in[:, lower:lower + per_block], exit_projector_matrix[tier_number, lower:lower + per_block], preferred_element_type=jnp.float32)
            mixed_sum = mixed_sum + lax.optimization_barrier(product.astype(jnp.bfloat16)).astype(jnp.float32)
        stream = (floats + mixed_sum).astype(jnp.bfloat16)
    return norm_rows(stream.astype(jnp.float32), finishing_rms_gains).astype(jnp.bfloat16)
```

```python
import functools
import math

import jax
import jax.numpy as jnp
from jax import lax
from jax.experimental import pallas as pl
from jax.experimental.pallas import tpu as pltpu
from jax.sharding import PartitionSpec as P


EPSILON = 1e-06
SQUASH_POWER = 8.0
LANES = 128
SUBLANES = 8
HALO = 16
F32 = jnp.float32
BF16 = jnp.bfloat16

HBM = pl.BlockSpec(memory_space=pltpu.MemorySpace.HBM)
VMEM = pl.BlockSpec(memory_space=pltpu.MemorySpace.VMEM)


def swap(value, axis, mask):
    count = lax.axis_size(axis)
    return lax.ppermute(value, axis, [(i, i ^ mask) for i in range(count)])


def shift(value, axis, steps):
    count = lax.axis_size(axis)
    return lax.ppermute(value, axis, [(i, i + steps) for i in range(count - steps)])


def spread(shard):
    groups = lax.axis_size("grp")
    count = lax.axis_size("sp")
    size = shard.shape[0] // groups
    mine = lax.dynamic_slice_in_dim(shard, lax.axis_index("grp") * size, size, 0)
    parts = [shard]
    crossed = [swap(mine, "sp", k) for k in range(1, count)]
    for arrived in crossed:
        parts.append(arrived)
        for q in range(1, groups):
            parts.append(swap(arrived, "grp", q))
    return parts


def gather_tp(own):
    held = {0: own}
    bit = lax.axis_size("tp") // 2
    while bit:
        for offset, value in list(held.items()):
            held[offset | bit] = swap(value, "tp", bit)
        bit //= 2
    return [held[k] for k in range(len(held))]


def start_parts(parts, scratch, sems, by_columns):
    groups, count = lax.axis_size("grp"), lax.axis_size("sp")
    g, s = lax.axis_index("grp"), lax.axis_index("sp")
    copies = []
    if len(parts) == 1:
        copies.append(pltpu.make_async_copy(parts[0], scratch, sems.at[0]))
    else:
        rows, cols = parts[0].shape
        step = rows // groups
        k = 1
        copies.append((parts[0], s, 0, rows))
        for d in range(1, count):
            for q in range(groups):
                copies.append((parts[k], s ^ d, (g ^ q) * step, step))
                k += 1
        made = []
        for i, (src, block, first, size) in enumerate(copies):
            if by_columns:
                dst = scratch.at[
                    pl.ds(pl.multiple_of(first, step), size),
                    pl.ds(pl.multiple_of(block * cols, LANES), cols),
                ]
            else:
                dst = scratch.at[pl.ds(pl.multiple_of(block * rows + first, step), size), :]
            made.append(pltpu.make_async_copy(src, dst, sems.at[i]))
        copies = made
    for c in copies:
        c.start()
    return copies


def recur_kernel(m, nw, *refs):
    xs, gain, ws = refs[:m], refs[m], refs[m + 1 : m + 1 + nw]
    normed, out, x_s, w_s, x_sem, w_sem = refs[m + 1 + nw :]
    t = lax.axis_index("tp")
    rows, width = x_s.shape
    c = width // m
    xc = []
    for j in range(m):
        dst = x_s.at[:, pl.ds(pl.multiple_of((t ^ j) * c, LANES), c)]
        xc.append(pltpu.make_async_copy(xs[j], dst, x_sem.at[j]))
    for copy in xc:
        copy.start()
    wc = start_parts(ws, w_s, w_sem, False)
    for copy in xc:
        copy.wait()
    chunk = 2 * SUBLANES

    def one(i, _):
        at = pl.ds(pl.multiple_of(i * chunk, chunk), chunk)
        x = x_s[at, :].astype(F32)
        mean = jnp.sum(x * x, axis=1, keepdims=True) * (1.0 / width)
        normed[at, :] = (x * lax.rsqrt(mean + EPSILON) * gain[...]).astype(BF16)
        return 0

    lax.fori_loop(0, rows // chunk, one, 0)
    for copy in wc:
        copy.wait()
    out[...] = jnp.dot(normed[...], w_s[...], preferred_element_type=F32).astype(BF16)


def branch_kernel(nw, *refs):
    normed, ws = refs[0], refs[1 : 1 + nw]
    out, w_s, w_sem = refs[1 + nw :]
    for copy in start_parts(ws, w_s, w_sem, False):
        copy.wait()
    rows = normed.shape[0]
    branch = jnp.dot(normed[...], w_s[...], preferred_element_type=F32)
    out[...] = jax.nn.gelu(branch.astype(BF16).astype(F32))


def one_minus_exp(y):
    series = y * (1.0 / 8.0) + 1.0
    for n in (7.0, 6.0, 5.0, 4.0, 3.0, 2.0):
        series = series * (y * (1.0 / n)) + 1.0
    return jnp.where(y > -0.3, -y * series, 1.0 - jnp.exp(y))


def scan_kernel(
    rec, halo, taps, valve_r, valve_i, rate, tmul, spike, acum, hcum, seg, tot, ext, conv, gate_r, gate_i
):
    rows, channels = rec.shape
    blocks = valve_r.shape[0]
    bw = channels // blocks
    ntap = taps.shape[0]
    ext[:HALO, :] = halo[...].astype(F32)
    ext[HALO:, :] = rec[...].astype(F32)
    chunk = 4 * SUBLANES
    for first in range(0, rows, chunk):
        acc = None
        for k in range(ntap):
            lo = HALO + first - (ntap - 1) + k
            term = ext[lo : lo + chunk, :] * taps[k : k + 1, :].astype(F32)
            acc = term if acc is None else acc + term
        conv[first : first + chunk, :] = acc.astype(BF16)
    for b in range(blocks):
        cols = slice(b * bw, (b + 1) * bw)
        gate_r[:, cols] = jnp.dot(conv[:, cols], valve_r[b], preferred_element_type=F32)
        gate_i[:, cols] = jnp.dot(conv[:, cols], valve_i[b], preferred_element_type=F32)
    step = 2 * SUBLANES

    def one(i, _):
        at = pl.ds(pl.multiple_of(i * step, step), step)
        reset = 0.5 * jnp.tanh(0.5 * gate_r[at, :]) + 0.5
        inject = 0.5 * jnp.tanh(0.5 * gate_i[at, :]) + 0.5
        logk = reset * rate[...] * tmul[at, :] + spike[at, :]
        keep = jnp.exp(logk)
        driven = inject * conv[at, :].astype(F32) * jnp.sqrt(one_minus_exp(2.0 * logk))
        for b in range(channels // LANES):
            lanes = slice(b * LANES, (b + 1) * LANES)
            acum[b, at, :] = keep[:, lanes]
            hcum[b, at, :] = driven[:, lanes]
        return 0

    lax.fori_loop(0, rows // step, one, 0)
    length = rows // SUBLANES

    def scan(i, carry):
        a_all, h_all = carry
        at = pl.ds(i, SUBLANES, stride=length)
        nxt_a, nxt_h = [], []
        for b in range(channels // LANES):
            a = acum[b, at, :]
            h = a * h_all[b] + hcum[b, at, :]
            aa = a * a_all[b]
            acum[b, at, :] = aa
            hcum[b, at, :] = h
            nxt_a.append(aa)
            nxt_h.append(h)
        return tuple(nxt_a), tuple(nxt_h)

    nl = channels // LANES
    ones = tuple(jnp.ones((SUBLANES, LANES), F32) for _ in range(nl))
    zeros = tuple(jnp.zeros((SUBLANES, LANES), F32) for _ in range(nl))
    a_all, h_all = lax.fori_loop(0, length, scan, (ones, zeros), unroll=4)
    for b in range(nl):
        lanes = slice(b * LANES, (b + 1) * LANES)
        ca, ch = jnp.ones((1, LANES), F32), jnp.zeros((1, LANES), F32)
        for i in range(SUBLANES):
            seg[i : i + 1, lanes] = ch
            seg[SUBLANES + i : SUBLANES + i + 1, lanes] = ca
            ch = a_all[b][i : i + 1, :] * ch + h_all[b][i : i + 1, :]
            ca = ca * a_all[b][i : i + 1, :]
        tot[0:1, lanes] = ca
        tot[1:2, lanes] = ch


def exit_kernel(m, nc, nw, *refs):
    gelu, acum, hcum, seg = refs[:4]
    before = refs[4 : 4 + nc]
    ws = refs[4 + nc : 4 + nc + nw]
    send, keep, mixed, w_s, w_sem = refs[4 + nc + nw :]
    copies = start_parts(ws, w_s, w_sem, True)
    rows, channels = gelu.shape
    t = lax.axis_index("tp")
    carry = jnp.zeros((1, channels), F32)
    for part in before:
        carry = part[0:1, :] * carry + part[1:2, :]
    entry = seg[0:SUBLANES, :] + seg[SUBLANES : 2 * SUBLANES, :] * carry
    length = rows // SUBLANES
    for i in range(SUBLANES):
        at = slice(i * length, (i + 1) * length)
        for b in range(channels // LANES):
            lanes = slice(b * LANES, (b + 1) * LANES)
            state = hcum[b, at, :] + acum[b, at, :] * entry[i : i + 1, lanes]
            mixed[at, lanes] = (gelu[at, lanes] * state).astype(BF16)
    for copy in copies:
        copy.wait()
    c = w_s.shape[1] // m
    for j in [k for k in range(m) if k & 1] + [k for k in range(m) if not k & 1]:
        w = w_s[:, pl.ds(pl.multiple_of((t ^ j) * c, LANES), c)]
        out = jnp.dot(mixed[...], w, preferred_element_type=F32).astype(BF16)
        (send if j & 1 else keep)[j >> 1] = out


def cost(flops, nbytes):
    return pl.CostEstimate(flops=int(flops), bytes_accessed=int(nbytes), transcendentals=0)


def on_device(
    starting_stream,
    multiplier_matrix,
    memory_path_matrix,
    filter_coefficients,
    memory_valve_matrix,
    entry_valve_matrix,
    forgetting_parameters,
    timestep_forgetting_multiplier,
    spike_extra,
    exit_projector_matrix,
    prelude_rms_gains,
    finishing_rms_gains,
):
    rows, own_width = starting_stream.shape
    layers, shard_rows, channels = memory_path_matrix.shape
    m = lax.axis_size("tp")
    n = lax.axis_size("sp")
    width = shard_rows * n
    shape = jax.ShapeDtypeStruct
    rates = -SQUASH_POWER * jax.nn.softplus(-forgetting_parameters)
    tmul = timestep_forgetting_multiplier[:, None]
    params = pltpu.CompilerParams(vmem_limit_bytes=48 * 1024 * 1024)

    path, mult, exits = [], [], []
    for layer in range(layers):
        path.append(spread(memory_path_matrix[layer]))
        mult.append(spread(multiplier_matrix[layer]))
        shard = exit_projector_matrix[layer]
        if shard.shape[1] % LANES:
            exits.append([lax.all_gather(shard, "sp", axis=1, tiled=True)])
        else:
            exits.append(spread(shard))

    own = starting_stream
    for layer in range(layers):
        pieces = gather_tp(own)
        ws = path[layer]
        normed, recurrent = pl.pallas_call(
            functools.partial(recur_kernel, m, len(ws)),
            out_shape=(shape((rows, width), BF16), shape((rows, channels), BF16)),
            in_specs=[HBM] * m + [VMEM] + [HBM] * len(ws),
            out_specs=(VMEM, VMEM),
            scratch_shapes=[
                pltpu.VMEM((rows, width), BF16),
                pltpu.VMEM((width, channels), BF16),
                pltpu.SemaphoreType.DMA((m,)),
                pltpu.SemaphoreType.DMA((len(ws),)),
            ],
            compiler_params=params,
            cost_estimate=cost(4 * rows * width * channels, 8 * rows * width),
            name="recur",
        )(*pieces, prelude_rms_gains[layer : layer + 1], *ws)
        halo = shift(recurrent[rows - HALO :], "sp", 1)
        ws = mult[layer]
        gelu = pl.pallas_call(
            functools.partial(branch_kernel, len(ws)),
            out_shape=shape((rows, channels), F32),
            in_specs=[VMEM] + [HBM] * len(ws),
            out_specs=VMEM,
            scratch_shapes=[
                pltpu.VMEM((width, channels), BF16),
                pltpu.SemaphoreType.DMA((len(ws),)),
            ],
            compiler_params=params,
            cost_estimate=cost(4 * rows * width * channels, 8 * rows * width),
            name="branch",
        )(normed, *ws)
        acum, hcum, seg, tot = pl.pallas_call(
            scan_kernel,
            out_shape=(
                shape((channels // LANES, rows, LANES), F32),
                shape((channels // LANES, rows, LANES), F32),
                shape((2 * SUBLANES, channels), F32),
                shape((2, channels), F32),
            ),
            in_specs=[VMEM] * 8,
            out_specs=(VMEM,) * 4,
            scratch_shapes=[
                pltpu.VMEM((HALO + rows, channels), F32),
                pltpu.VMEM((rows, channels), BF16),
                pltpu.VMEM((rows, channels), F32),
                pltpu.VMEM((rows, channels), F32),
            ],
            compiler_params=params,
            cost_estimate=cost(8 * rows * width * channels, 8 * rows * width),
            name="scan",
        )(
            recurrent,
            halo,
            filter_coefficients[layer],
            memory_valve_matrix[layer],
            entry_valve_matrix[layer],
            rates[layer : layer + 1],
            tmul,
            spike_extra,
        )
        before = [shift(tot, "sp", k) for k in range(n - 1, 0, -1)]
        ws = exits[layer]
        send, keep = pl.pallas_call(
            functools.partial(exit_kernel, m, len(before), len(ws)),
            out_shape=(
                shape((m // 2, rows, own_width), BF16),
                shape((m - m // 2, rows, own_width), BF16),
            ),
            in_specs=[VMEM] * (4 + len(before)) + [HBM] * len(ws),
            out_specs=(VMEM, VMEM),
            scratch_shapes=[
                pltpu.VMEM((rows, channels), BF16),
                pltpu.VMEM((channels, width), BF16),
                pltpu.SemaphoreType.DMA((len(ws),)),
            ],
            compiler_params=params,
            cost_estimate=cost(4 * rows * width * channels, 8 * rows * width),
            name="exit",
        )(gelu, acum, hcum, seg, *before, *ws)
        bit = 1
        while True:
            arrived = swap(send, "tp", bit)
            total = keep.astype(F32) + arrived.astype(F32)
            bit *= 2
            if bit == m:
                break
            send, keep = total[1::2].astype(BF16), total[0::2]
        own = (own.astype(F32) + total[0]).astype(BF16)
    floats = own.astype(F32)
    squares = jnp.sum(floats * floats, axis=1)
    bit = 1
    while bit < m:
        squares = squares + swap(squares, "tp", bit)
        bit *= 2
    inv_rms = lax.rsqrt(squares / width + EPSILON)
    return (floats * inv_rms[:, None] * finishing_rms_gains[None, :]).astype(BF16)


def solution(mesh):
    return jax.shard_map(
        on_device,
        mesh=mesh,
        in_specs=(
            P(("grp", "sp"), "tp"),
            P(None, "sp", "tp"),
            P(None, "sp", "tp"),
            P(None, None, "tp"),
            P(None, "tp", None, None),
            P(None, "tp", None, None),
            P(None, "tp"),
            P(("grp", "sp")),
            P(("grp", "sp"), "tp"),
            P(None, "tp", "sp"),
            P(),
            P("tp"),
        ),
        out_specs=P(("grp", "sp"), "tp"),
        check_vma=False,
    )
```

```python
import functools

import jax
import jax.numpy as jnp
from jax import lax
from jax.experimental import pallas as pl
from jax.experimental.pallas import tpu as pltpu
from jax.sharding import PartitionSpec as P


EPSILON = 1e-06
SQUASH_POWER = 8.0
LANES = 128
SUBLANES = 8
HALO = 16
F32 = jnp.float32
BF16 = jnp.bfloat16

HBM = pl.BlockSpec(memory_space=pltpu.MemorySpace.HBM)
VMEM = pl.BlockSpec(memory_space=pltpu.MemorySpace.VMEM)


def swap(value, axis, mask):
    count = lax.axis_size(axis)
    return lax.ppermute(value, axis, [(i, i ^ mask) for i in range(count)])


def shift(value, axis, steps):
    count = lax.axis_size(axis)
    return lax.ppermute(value, axis, [(i, i + steps) for i in range(count - steps)])


def spread(matrices, layer, by_sp):
    groups = lax.axis_size("grp")
    count = lax.axis_size("sp")
    size, cols = matrices[0].shape[1] // groups, matrices[0].shape[2]
    first = lax.axis_index("grp") * size
    own = [lax.dynamic_slice(w, (layer, first, 0), (1, size, cols)) for w in matrices]
    mine = jnp.concatenate(own, axis=0)
    held, source = {0: mine}, {}
    bit = count // 2
    while bit:
        for offset, value in sorted(held.items()):
            held[offset | bit] = swap(value, "sp", bit)
            source[offset | bit] = (offset, bit)
        bit //= 2
    parts, others = [], {}
    for k in range(1, count):
        parts.append(held[k])
        for q in range(1, groups):
            offset, bit = source[k]
            if by_sp and offset:
                others[k, q] = swap(others[offset, q], "sp", bit)
            else:
                others[k, q] = swap(held[k], "grp", q)
            parts.append(others[k, q])
    return parts


def gather_tp(own):
    held = {0: own}
    bit = lax.axis_size("tp") // 2
    while bit:
        for offset, value in list(held.items()):
            held[offset | bit] = swap(value, "tp", bit)
        bit //= 2
    return [held[k] for k in range(len(held))]


def start_parts(layer, place, whole, parts, scratch, sems, by_columns):
    if not parts:
        copies = [pltpu.make_async_copy(whole, scratch, sems.at[0])]
        copies[0].start()
        return copies
    groups, count = lax.axis_size("grp"), lax.axis_size("sp")
    g, s = lax.axis_index("grp"), lax.axis_index("sp")
    _, rows, cols = whole.shape
    step = rows // groups
    plan = [(whole.at[layer], s, 0, rows)]
    k = 0
    for d in range(1, count):
        for q in range(groups):
            plan.append((parts[k].at[place], s ^ d, (g ^ q) * step, step))
            k += 1
    copies = []
    for i, (src, block, first, size) in enumerate(plan):
        if by_columns:
            dst = scratch.at[
                pl.ds(pl.multiple_of(first, step), size),
                pl.ds(pl.multiple_of(block * cols, LANES), cols),
            ]
        else:
            dst = scratch.at[pl.ds(pl.multiple_of(block * rows + first, step), size), :]
        copies.append(pltpu.make_async_copy(src, dst, sems.at[i]))
    for c in copies:
        c.start()
    return copies


def recur_kernel(layer, place, m, nw, *refs):
    xs, gain, ws = refs[:m], refs[m], refs[m + 1 : m + 1 + nw]
    normed, out, x_s, w_s, x_sem, w_sem = refs[m + 1 + nw :]
    t = lax.axis_index("tp")
    rows, width = x_s.shape
    c = width // m
    xc = []
    for j in range(m):
        dst = x_s.at[:, pl.ds(pl.multiple_of((t ^ j) * c, LANES), c)]
        xc.append(pltpu.make_async_copy(xs[j], dst, x_sem.at[j]))
    for copy in xc:
        copy.start()
    wc = start_parts(layer, place, ws[0], ws[1:], w_s, w_sem, False)
    for copy in xc:
        copy.wait()
    chunk = 2 * SUBLANES

    def one(i, _):
        at = pl.ds(pl.multiple_of(i * chunk, chunk), chunk)
        x = x_s[at, :].astype(F32)
        mean = jnp.sum(x * x, axis=1, keepdims=True) * (1.0 / width)
        normed[at, :] = (x * lax.rsqrt(mean + EPSILON) * gain[...]).astype(BF16)
        return 0

    lax.fori_loop(0, rows // chunk, one, 0, unroll=5 if rows // chunk % 5 == 0 else 4)
    for copy in wc:
        copy.wait()
    out[...] = jnp.dot(normed[...], w_s[...], preferred_element_type=F32).astype(BF16)


def branch_kernel(layer, place, pre, nw, *refs):
    normed, ws = refs[0], refs[1 : 1 + nw]
    out, w_s, w_sem = refs[1 + nw :]
    for copy in start_parts(layer, place, ws[0], ws[1:], w_s, w_sem, False):
        copy.wait()
    branch = jnp.dot(normed[pre:, :], w_s[...], preferred_element_type=F32)
    out[...] = jax.nn.gelu(branch.astype(BF16).astype(F32))


def one_minus_exp(y):
    series = y * (1.0 / 8.0) + 1.0
    for n in (7.0, 6.0, 5.0, 4.0, 3.0, 2.0):
        series = series * (y * (1.0 / n)) + 1.0
    return jnp.where(y > -0.3, -y * series, 1.0 - jnp.exp(y))


def scan_kernel(pre, *refs):
    rec, refs = refs[0], refs[1:]
    if pre == 0:
        halo, refs = refs[0], refs[1:]
    taps, valve_r, valve_i, rate, tmul, spike = refs[:6]
    acum, hcum, seg, tot, ext, conv, gate_r, gate_i, spike_s, sem = refs[6:]
    rows, channels = spike.shape
    fetch = pltpu.make_async_copy(spike, spike_s, sem.at[0])
    fetch.start()
    blocks = valve_r.shape[0]
    bw = channels // blocks
    ntap = taps.shape[0]
    if pre == 0:
        ext[:HALO, :] = halo[...].astype(F32)
    ext[HALO - pre :, :] = rec[...].astype(F32)
    chunk = 4 * SUBLANES
    for first in range(0, rows, chunk):
        acc = None
        for k in range(ntap):
            lo = HALO + first - (ntap - 1) + k
            term = ext[lo : lo + chunk, :] * taps[k : k + 1, :].astype(F32)
            acc = term if acc is None else acc + term
        conv[first : first + chunk, :] = acc.astype(BF16)
    for b in range(blocks):
        cols = slice(b * bw, (b + 1) * bw)
        gate_r[:, cols] = jnp.dot(conv[:, cols], valve_r[b], preferred_element_type=F32)
        gate_i[:, cols] = jnp.dot(conv[:, cols], valve_i[b], preferred_element_type=F32)
    step = 2 * SUBLANES
    fetch.wait()

    def one(i, _):
        at = pl.ds(pl.multiple_of(i * step, step), step)
        reset = 0.5 * jnp.tanh(0.5 * gate_r[at, :]) + 0.5
        inject = 0.5 * jnp.tanh(0.5 * gate_i[at, :]) + 0.5
        logk = reset * rate[...] * tmul[at, :] + spike_s[at, :]
        keep = jnp.exp(logk)
        driven = inject * conv[at, :].astype(F32) * jnp.sqrt(one_minus_exp(2.0 * logk))
        for b in range(channels // LANES):
            lanes = slice(b * LANES, (b + 1) * LANES)
            acum[b, at, :] = keep[:, lanes]
            hcum[b, at, :] = driven[:, lanes]
        return 0

    lax.fori_loop(0, rows // step, one, 0, unroll=2)
    length = rows // SUBLANES

    def scan(i, carry):
        a_all, h_all = carry
        at = pl.ds(i, SUBLANES, stride=length)
        nxt_a, nxt_h = [], []
        for b in range(channels // LANES):
            a = acum[b, at, :]
            h = a * h_all[b] + hcum[b, at, :]
            aa = a * a_all[b]
            acum[b, at, :] = aa
            hcum[b, at, :] = h
            nxt_a.append(aa)
            nxt_h.append(h)
        return tuple(nxt_a), tuple(nxt_h)

    nl = channels // LANES
    ones = tuple(jnp.ones((SUBLANES, LANES), F32) for _ in range(nl))
    zeros = tuple(jnp.zeros((SUBLANES, LANES), F32) for _ in range(nl))
    a_all, h_all = lax.fori_loop(0, length, scan, (ones, zeros), unroll=4)
    for b in range(nl):
        lanes = slice(b * LANES, (b + 1) * LANES)
        ca, ch = jnp.ones((1, LANES), F32), jnp.zeros((1, LANES), F32)
        for i in range(SUBLANES):
            seg[i : i + 1, lanes] = ch
            seg[SUBLANES + i : SUBLANES + i + 1, lanes] = ca
            ch = a_all[b][i : i + 1, :] * ch + h_all[b][i : i + 1, :]
            ca = ca * a_all[b][i : i + 1, :]
        tot[0:1, lanes] = ca
        tot[1:2, lanes] = ch


def exit_kernel(layer, place, m, nc, nw, *refs):
    gelu, acum, hcum, seg = refs[:4]
    before = refs[4 : 4 + nc]
    ws = refs[4 + nc : 4 + nc + nw]
    send, keep, mixed, w_s, w_sem = refs[4 + nc + nw :]
    copies = start_parts(layer, place, ws[0], ws[1:], w_s, w_sem, True)
    rows, channels = gelu.shape
    t = lax.axis_index("tp")
    carry = jnp.zeros((1, channels), F32)
    for part in before:
        carry = part[0:1, :] * carry + part[1:2, :]
    entry = seg[0:SUBLANES, :] + seg[SUBLANES : 2 * SUBLANES, :] * carry
    length = rows // SUBLANES
    for i in range(SUBLANES):
        at = slice(i * length, (i + 1) * length)
        for b in range(channels // LANES):
            lanes = slice(b * LANES, (b + 1) * LANES)
            state = hcum[b, at, :] + acum[b, at, :] * entry[i : i + 1, lanes]
            mixed[at, lanes] = (gelu[at, lanes] * state).astype(BF16)
    for copy in copies:
        copy.wait()
    c = w_s.shape[1] // m
    for j in [k for k in range(m) if k & 1] + [k for k in range(m) if not k & 1]:
        w = w_s[:, pl.ds(pl.multiple_of((t ^ j) * c, LANES), c)]
        out = jnp.dot(mixed[...], w, preferred_element_type=F32).astype(BF16)
        (send if j & 1 else keep)[j >> 1] = out


def cost(flops, nbytes):
    return pl.CostEstimate(flops=int(flops), bytes_accessed=int(nbytes), transcendentals=0)


def on_device(
    starting_stream,
    multiplier_matrix,
    memory_path_matrix,
    filter_coefficients,
    memory_valve_matrix,
    entry_valve_matrix,
    forgetting_parameters,
    timestep_forgetting_multiplier,
    spike_extra,
    exit_projector_matrix,
    prelude_rms_gains,
    finishing_rms_gains,
):
    rows, own_width = starting_stream.shape
    layers, shard_rows, channels = memory_path_matrix.shape
    m = lax.axis_size("tp")
    n = lax.axis_size("sp")
    width = shard_rows * n
    shape = jax.ShapeDtypeStruct
    rates = -SQUASH_POWER * jax.nn.softplus(-forgetting_parameters)
    tmul = timestep_forgetting_multiplier[:, None]
    params = pltpu.CompilerParams(vmem_limit_bytes=16 * 1024 * 1024)

    chunks, places = {}, {}
    named = {"m": memory_path_matrix, "b": multiplier_matrix, "e": exit_projector_matrix}
    for layer in range(layers):
        groups = ["m", "b", "e"]
        if named["e"].shape[2] % LANES:
            shard = named["e"][layer]
            chunks[f"e{layer}"] = [lax.all_gather(shard, "sp", axis=1, tiled=True)]
            places[f"e{layer}"] = 0
            groups = ["m", "b"]
        for kinds in groups:
            matrices = [named[kind] for kind in kinds]
            parts = spread(matrices, layer, kinds == "e" and layer == layers - 1)
            for place, kind in enumerate(kinds):
                chunks[f"{kind}{layer}"] = [named[kind]] + parts
                places[f"{kind}{layer}"] = place

    own = starting_stream
    for layer in range(layers):
        pre = HALO if layer == 0 else 0
        lead = [shift(own[rows - HALO :], "sp", 1)] if pre else []
        pieces = gather_tp(jnp.concatenate(lead + [own], axis=0))
        ws = chunks[f"m{layer}"]
        normed, recurrent = pl.pallas_call(
            functools.partial(recur_kernel, layer, places[f"m{layer}"], m, len(ws)),
            out_shape=(
                shape((pre + rows, width), BF16),
                shape((pre + rows, channels), BF16),
            ),
            in_specs=[HBM] * m + [VMEM] + [HBM] * len(ws),
            out_specs=(VMEM, VMEM),
            scratch_shapes=[
                pltpu.VMEM((pre + rows, width), BF16),
                pltpu.VMEM((width, channels), BF16),
                pltpu.SemaphoreType.DMA((m,)),
                pltpu.SemaphoreType.DMA((len(ws),)),
            ],
            compiler_params=params,
            cost_estimate=cost(4 * rows * width * channels, 8 * rows * width),
            name="recur",
        )(*pieces, prelude_rms_gains[layer : layer + 1], *ws)
        halo = []
        if not pre:
            halo = [shift(recurrent[rows - HALO :], "sp", 1)]
        ws = chunks[f"b{layer}"]
        gelu = pl.pallas_call(
            functools.partial(branch_kernel, layer, places[f"b{layer}"], pre, len(ws)),
            out_shape=shape((rows, channels), F32),
            in_specs=[VMEM] + [HBM] * len(ws),
            out_specs=VMEM,
            scratch_shapes=[
                pltpu.VMEM((width, channels), BF16),
                pltpu.SemaphoreType.DMA((len(ws),)),
            ],
            compiler_params=params,
            cost_estimate=cost(4 * rows * width * channels, 8 * rows * width),
            name="branch",
        )(normed, *ws)
        acum, hcum, seg, tot = pl.pallas_call(
            functools.partial(scan_kernel, pre),
            out_shape=(
                shape((channels // LANES, rows, LANES), F32),
                shape((channels // LANES, rows, LANES), F32),
                shape((2 * SUBLANES, channels), F32),
                shape((2, channels), F32),
            ),
            in_specs=[VMEM] * (6 + len(halo)) + [HBM],
            out_specs=(VMEM,) * 4,
            scratch_shapes=[
                pltpu.VMEM((HALO + rows, channels), F32),
                pltpu.VMEM((rows, channels), BF16),
                pltpu.VMEM((rows, channels), F32),
                pltpu.VMEM((rows, channels), F32),
                pltpu.VMEM((rows, channels), F32),
                pltpu.SemaphoreType.DMA((1,)),
            ],
            compiler_params=params,
            cost_estimate=cost(8 * rows * width * channels, 8 * rows * width),
            name="scan",
        )(
            recurrent,
            *halo,
            filter_coefficients[layer],
            memory_valve_matrix[layer],
            entry_valve_matrix[layer],
            rates[layer : layer + 1],
            tmul,
            spike_extra,
        )
        before = [shift(tot, "sp", k) for k in range(n - 1, 0, -1)]
        ws = chunks[f"e{layer}"]
        send, keep = pl.pallas_call(
            functools.partial(exit_kernel, layer, places[f"e{layer}"], m, len(before), len(ws)),
            out_shape=(
                shape((m // 2, rows, own_width), BF16),
                shape((m - m // 2, rows, own_width), BF16),
            ),
            in_specs=[VMEM] * (4 + len(before)) + [HBM] * len(ws),
            out_specs=(VMEM, VMEM),
            scratch_shapes=[
                pltpu.VMEM((rows, channels), BF16),
                pltpu.VMEM((channels, width), BF16),
                pltpu.SemaphoreType.DMA((len(ws),)),
            ],
            compiler_params=params,
            cost_estimate=cost(4 * rows * width * channels, 8 * rows * width),
            name="exit",
        )(gelu, acum, hcum, seg, *before, *ws)
        bit = 1
        while True:
            arrived = swap(send, "tp", bit)
            total = keep.astype(F32) + arrived.astype(F32)
            bit *= 2
            if bit == m:
                break
            send, keep = total[1::2].astype(BF16), total[0::2]
        own = (own.astype(F32) + total[0]).astype(BF16)
    floats = own.astype(F32)
    squares = jnp.sum(floats * floats, axis=1)
    squares = sum([swap(squares, "tp", k) for k in range(1, m)], squares)
    inv_rms = lax.rsqrt(squares / width + EPSILON)
    return (floats * inv_rms[:, None] * finishing_rms_gains[None, :]).astype(BF16)


def solution(mesh):
    def step(*args):
        run = jax.shard_map(
            on_device,
            mesh=mesh,
            in_specs=(
                P(("grp", "sp"), "tp"),
                P(None, "sp", "tp"),
                P(None, "sp", "tp"),
                P(None, None, "tp"),
                P(None, "tp", None, None),
                P(None, "tp", None, None),
                P(None, "tp"),
                P(("grp", "sp")),
                P(("grp", "sp"), "tp"),
                P(None, "tp", "sp"),
                P(),
                P("tp"),
            ),
            out_specs=P(("grp", "sp"), "tp"),
            check_vma=False,
        )
        jax.eval_shape(run, *args)
        return run(*args)

    return step
```

```python
import functools

import jax
import jax.numpy as jnp
from jax import lax
from jax.experimental import pallas as pl
from jax.experimental.pallas import tpu as pltpu
from jax.sharding import PartitionSpec as P


EPSILON = 1e-06
SQUASH_POWER = 8.0
LANES = 128
SUBLANES = 8
HALO = 16
F32 = jnp.float32
BF16 = jnp.bfloat16

HBM = pl.BlockSpec(memory_space=pltpu.MemorySpace.HBM)
VMEM = pl.BlockSpec(memory_space=pltpu.MemorySpace.VMEM)


def swap(value, axis, mask):
    count = lax.axis_size(axis)
    return lax.ppermute(value, axis, [(i, i ^ mask) for i in range(count)])


def shift(value, axis, steps):
    count = lax.axis_size(axis)
    return lax.ppermute(value, axis, [(i, i + steps) for i in range(count - steps)])


def spread(matrices, layer, by_sp):
    groups = lax.axis_size("grp")
    count = lax.axis_size("sp")
    size, cols = matrices[0].shape[1] // groups, matrices[0].shape[2]
    first = lax.axis_index("grp") * size
    own = [lax.dynamic_slice(w, (layer, first, 0), (1, size, cols)) for w in matrices]
    mine = jnp.concatenate(own, axis=0)
    held, source = {0: mine}, {}
    bit = count // 2
    while bit:
        for offset, value in sorted(held.items()):
            held[offset | bit] = swap(value, "sp", bit)
            source[offset | bit] = (offset, bit)
        bit //= 2
    parts, others = [], {}
    for k in range(1, count):
        parts.append(held[k])
        for q in range(1, groups):
            offset, bit = source[k]
            if by_sp and offset:
                others[k, q] = swap(others[offset, q], "sp", bit)
            else:
                others[k, q] = swap(held[k], "grp", q)
            parts.append(others[k, q])
    return parts


def gather_tp(own, far=None):
    held = {0: own}
    bit = lax.axis_size("tp") // 2
    if far is not None:
        held[bit] = far
        bit //= 2
    while bit:
        for offset, value in list(held.items()):
            held[offset | bit] = swap(value, "tp", bit)
        bit //= 2
    return [held[k] for k in range(len(held))]


def start_parts(layer, place, whole, parts, scratch, sems, by_columns):
    if not parts:
        copies = [pltpu.make_async_copy(whole, scratch, sems.at[0])]
        copies[0].start()
        return copies
    groups, count = lax.axis_size("grp"), lax.axis_size("sp")
    g, s = lax.axis_index("grp"), lax.axis_index("sp")
    _, rows, cols = whole.shape
    step = rows // groups
    plan = [(whole.at[layer], s, 0, rows)]
    k = 0
    for d in range(1, count):
        for q in range(groups):
            plan.append((parts[k].at[place], s ^ d, (g ^ q) * step, step))
            k += 1
    copies = []
    for i, (src, block, first, size) in enumerate(plan):
        if by_columns:
            dst = scratch.at[
                pl.ds(pl.multiple_of(first, step), size),
                pl.ds(pl.multiple_of(block * cols, LANES), cols),
            ]
        else:
            dst = scratch.at[pl.ds(pl.multiple_of(block * rows + first, step), size), :]
        copies.append(pltpu.make_async_copy(src, dst, sems.at[i]))
    for c in copies:
        c.start()
    return copies


def recur_kernel(layer, place, m, nw, *refs):
    xs, gain, ws = refs[:m], refs[m], refs[m + 1 : m + 1 + nw]
    normed, out, x_s, w_s, x_sem, w_sem = refs[m + 1 + nw :]
    t = lax.axis_index("tp")
    rows, width = x_s.shape
    c = width // m
    xc = []
    for j in range(m):
        dst = x_s.at[:, pl.ds(pl.multiple_of((t ^ j) * c, LANES), c)]
        xc.append(pltpu.make_async_copy(xs[j], dst, x_sem.at[j]))
    for copy in xc:
        copy.start()
    wc = start_parts(layer, place, ws[0], ws[1:], w_s, w_sem, False)
    for copy in xc:
        copy.wait()
    chunk = 2 * SUBLANES

    def one(i, _):
        at = pl.ds(pl.multiple_of(i * chunk, chunk), chunk)
        x = x_s[at, :].astype(F32)
        mean = jnp.sum(x * x, axis=1, keepdims=True) * (1.0 / width)
        normed[at, :] = (x * lax.rsqrt(mean + EPSILON) * gain[...]).astype(BF16)
        return 0

    lax.fori_loop(0, rows // chunk, one, 0, unroll=5 if rows // chunk % 5 == 0 else 4)
    for copy in wc:
        copy.wait()
    out[...] = jnp.dot(normed[...], w_s[...], preferred_element_type=F32).astype(BF16)


def branch_kernel(layer, place, pre, nw, *refs):
    normed, ws = refs[0], refs[1 : 1 + nw]
    out, w_s, w_sem = refs[1 + nw :]
    for copy in start_parts(layer, place, ws[0], ws[1:], w_s, w_sem, False):
        copy.wait()
    branch = jnp.dot(normed[pre:, :], w_s[...], preferred_element_type=F32)
    out[...] = jax.nn.gelu(branch.astype(BF16).astype(F32))


def one_minus_exp(y):
    series = y * (1.0 / 8.0) + 1.0
    for n in (7.0, 6.0, 5.0, 4.0, 3.0, 2.0):
        series = series * (y * (1.0 / n)) + 1.0
    return jnp.where(y > -0.3, -y * series, 1.0 - jnp.exp(y))


def scan_kernel(pre, *refs):
    rec, refs = refs[0], refs[1:]
    if pre == 0:
        halo, refs = refs[0], refs[1:]
    taps, valve_r, valve_i, rate, tmul, spike = refs[:6]
    acum, hcum, seg, tot, ext, conv, gate_r, gate_i, spike_s, sem = refs[6:]
    rows, channels = spike.shape
    fetch = pltpu.make_async_copy(spike, spike_s, sem.at[0])
    fetch.start()
    blocks = valve_r.shape[0]
    bw = channels // blocks
    ntap = taps.shape[0]
    if pre == 0:
        ext[:HALO, :] = halo[...].astype(F32)
    ext[HALO - pre :, :] = rec[...].astype(F32)
    chunk = 4 * SUBLANES
    for first in range(0, rows, chunk):
        acc = None
        for k in range(ntap):
            lo = HALO + first - (ntap - 1) + k
            term = ext[lo : lo + chunk, :] * taps[k : k + 1, :].astype(F32)
            acc = term if acc is None else acc + term
        conv[first : first + chunk, :] = acc.astype(BF16)
    for b in range(blocks):
        cols = slice(b * bw, (b + 1) * bw)
        gate_r[:, cols] = jnp.dot(conv[:, cols], valve_r[b], preferred_element_type=F32)
        gate_i[:, cols] = jnp.dot(conv[:, cols], valve_i[b], preferred_element_type=F32)
    step = 2 * SUBLANES
    fetch.wait()

    def one(i, _):
        at = pl.ds(pl.multiple_of(i * step, step), step)
        reset = 0.5 * jnp.tanh(0.5 * gate_r[at, :]) + 0.5
        inject = 0.5 * jnp.tanh(0.5 * gate_i[at, :]) + 0.5
        logk = reset * rate[...] * tmul[at, :] + spike_s[at, :]
        keep = jnp.exp(logk)
        driven = inject * conv[at, :].astype(F32) * jnp.sqrt(one_minus_exp(2.0 * logk))
        for b in range(channels // LANES):
            lanes = slice(b * LANES, (b + 1) * LANES)
            acum[b, at, :] = keep[:, lanes]
            hcum[b, at, :] = driven[:, lanes]
        return 0

    lax.fori_loop(0, rows // step, one, 0, unroll=4)
    length = rows // SUBLANES

    def scan(i, carry):
        a_all, h_all = carry
        at = pl.ds(i, SUBLANES, stride=length)
        nxt_a, nxt_h = [], []
        for b in range(channels // LANES):
            a = acum[b, at, :]
            h = a * h_all[b] + hcum[b, at, :]
            aa = a * a_all[b]
            acum[b, at, :] = aa
            hcum[b, at, :] = h
            nxt_a.append(aa)
            nxt_h.append(h)
        return tuple(nxt_a), tuple(nxt_h)

    nl = channels // LANES
    ones = tuple(jnp.ones((SUBLANES, LANES), F32) for _ in range(nl))
    zeros = tuple(jnp.zeros((SUBLANES, LANES), F32) for _ in range(nl))
    a_all, h_all = lax.fori_loop(0, length, scan, (ones, zeros), unroll=8)
    for b in range(nl):
        lanes = slice(b * LANES, (b + 1) * LANES)
        ca, ch = jnp.ones((1, LANES), F32), jnp.zeros((1, LANES), F32)
        for i in range(SUBLANES):
            seg[i : i + 1, lanes] = ch
            seg[SUBLANES + i : SUBLANES + i + 1, lanes] = ca
            ch = a_all[b][i : i + 1, :] * ch + h_all[b][i : i + 1, :]
            ca = ca * a_all[b][i : i + 1, :]
        tot[0:1, lanes] = ca
        tot[1:2, lanes] = ch


def exit_kernel(layer, place, m, nc, nw, *refs):
    gelu, acum, hcum, seg = refs[:4]
    before = refs[4 : 4 + nc]
    ws = refs[4 + nc : 4 + nc + nw]
    send, keep, mixed, w_s, w_sem = refs[4 + nc + nw :]
    copies = start_parts(layer, place, ws[0], ws[1:], w_s, w_sem, True)
    rows, channels = gelu.shape
    t = lax.axis_index("tp")
    carry = jnp.zeros((1, channels), F32)
    for part in before:
        carry = part[0:1, :] * carry + part[1:2, :]
    entry = seg[0:SUBLANES, :] + seg[SUBLANES : 2 * SUBLANES, :] * carry
    length = rows // SUBLANES
    for i in range(SUBLANES):
        at = slice(i * length, (i + 1) * length)
        for b in range(channels // LANES):
            lanes = slice(b * LANES, (b + 1) * LANES)
            state = hcum[b, at, :] + acum[b, at, :] * entry[i : i + 1, lanes]
            mixed[at, lanes] = (gelu[at, lanes] * state).astype(BF16)
    for copy in copies:
        copy.wait()
    c = w_s.shape[1] // m
    for j in [k for k in range(m) if k & 1] + [k for k in range(m) if not k & 1]:
        w = w_s[:, pl.ds(pl.multiple_of((t ^ j) * c, LANES), c)]
        out = jnp.dot(mixed[...], w, preferred_element_type=F32).astype(BF16)
        (send if j & 1 else keep)[j >> 1] = out


def cost(flops, nbytes):
    return pl.CostEstimate(flops=int(flops), bytes_accessed=int(nbytes), transcendentals=0)


def on_device(
    starting_stream,
    multiplier_matrix,
    memory_path_matrix,
    filter_coefficients,
    memory_valve_matrix,
    entry_valve_matrix,
    forgetting_parameters,
    timestep_forgetting_multiplier,
    spike_extra,
    exit_projector_matrix,
    prelude_rms_gains,
    finishing_rms_gains,
):
    rows, own_width = starting_stream.shape
    layers, shard_rows, channels = memory_path_matrix.shape
    m = lax.axis_size("tp")
    n = lax.axis_size("sp")
    width = shard_rows * n
    shape = jax.ShapeDtypeStruct
    rates = -SQUASH_POWER * jax.nn.softplus(-forgetting_parameters)
    tmul = timestep_forgetting_multiplier[:, None]
    params = pltpu.CompilerParams(vmem_limit_bytes=16 * 1024 * 1024)

    chunks, places = {}, {}
    named = {"m": memory_path_matrix, "b": multiplier_matrix, "e": exit_projector_matrix}
    for layer in range(layers):
        groups = ["m", "b", "e"]
        if named["e"].shape[2] % LANES:
            shard = named["e"][layer]
            chunks[f"e{layer}"] = [lax.all_gather(shard, "sp", axis=1, tiled=True)]
            places[f"e{layer}"] = 0
            groups = ["m", "b"]
        for kinds in groups:
            matrices = [named[kind] for kind in kinds]
            parts = spread(matrices, layer, kinds == "e" and layer == layers - 1)
            for place, kind in enumerate(kinds):
                chunks[f"{kind}{layer}"] = [named[kind]] + parts
                places[f"{kind}{layer}"] = place

    own, far = starting_stream, None
    for layer in range(layers):
        pre = HALO if layer == 0 else 0
        lead = [shift(own[rows - HALO :], "sp", 1)] if pre else []
        pieces = gather_tp(jnp.concatenate(lead + [own], axis=0), far)
        ws = chunks[f"m{layer}"]
        normed, recurrent = pl.pallas_call(
            functools.partial(recur_kernel, layer, places[f"m{layer}"], m, len(ws)),
            out_shape=(
                shape((pre + rows, width), BF16),
                shape((pre + rows, channels), BF16),
            ),
            in_specs=[HBM] * m + [VMEM] + [HBM] * len(ws),
            out_specs=(VMEM, VMEM),
            scratch_shapes=[
                pltpu.VMEM((pre + rows, width), BF16),
                pltpu.VMEM((width, channels), BF16),
                pltpu.SemaphoreType.DMA((m,)),
                pltpu.SemaphoreType.DMA((len(ws),)),
            ],
            compiler_params=params,
            cost_estimate=cost(4 * rows * width * channels, 8 * rows * width),
            name="recur",
        )(*pieces, prelude_rms_gains[layer : layer + 1], *ws)
        halo = []
        if not pre:
            halo = [shift(recurrent[rows - HALO :], "sp", 1)]
        ws = chunks[f"b{layer}"]
        gelu = pl.pallas_call(
            functools.partial(branch_kernel, layer, places[f"b{layer}"], pre, len(ws)),
            out_shape=shape((rows, channels), F32),
            in_specs=[VMEM] + [HBM] * len(ws),
            out_specs=VMEM,
            scratch_shapes=[
                pltpu.VMEM((width, channels), BF16),
                pltpu.SemaphoreType.DMA((len(ws),)),
            ],
            compiler_params=params,
            cost_estimate=cost(4 * rows * width * channels, 8 * rows * width),
            name="branch",
        )(normed, *ws)
        acum, hcum, seg, tot = pl.pallas_call(
            functools.partial(scan_kernel, pre),
            out_shape=(
                shape((channels // LANES, rows, LANES), F32),
                shape((channels // LANES, rows, LANES), F32),
                shape((2 * SUBLANES, channels), F32),
                shape((2, channels), F32),
            ),
            in_specs=[VMEM] * (6 + len(halo)) + [HBM],
            out_specs=(VMEM,) * 4,
            scratch_shapes=[
                pltpu.VMEM((HALO + rows, channels), F32),
                pltpu.VMEM((rows, channels), BF16),
                pltpu.VMEM((rows, channels), F32),
                pltpu.VMEM((rows, channels), F32),
                pltpu.VMEM((rows, channels), F32),
                pltpu.SemaphoreType.DMA((1,)),
            ],
            compiler_params=params,
            cost_estimate=cost(8 * rows * width * channels, 8 * rows * width),
            name="scan",
        )(
            recurrent,
            *halo,
            filter_coefficients[layer],
            memory_valve_matrix[layer],
            entry_valve_matrix[layer],
            rates[layer : layer + 1],
            tmul,
            spike_extra,
        )
        before = [shift(tot, "sp", k) for k in range(n - 1, 0, -1)]
        ws = chunks[f"e{layer}"]
        send, keep = pl.pallas_call(
            functools.partial(exit_kernel, layer, places[f"e{layer}"], m, len(before), len(ws)),
            out_shape=(
                shape((m // 2, rows, own_width), BF16),
                shape((m - m // 2, rows, own_width), BF16),
            ),
            in_specs=[VMEM] * (4 + len(before)) + [HBM] * len(ws),
            out_specs=(VMEM, VMEM),
            scratch_shapes=[
                pltpu.VMEM((rows, channels), BF16),
                pltpu.VMEM((channels, width), BF16),
                pltpu.SemaphoreType.DMA((len(ws),)),
            ],
            compiler_params=params,
            cost_estimate=cost(4 * rows * width * channels, 8 * rows * width),
            name="exit",
        )(gelu, acum, hcum, seg, *before, *ws)
        bit = 1
        while bit < m // 2:
            arrived = swap(send, "tp", bit)
            total = keep.astype(F32) + arrived.astype(F32)
            send, keep = total[1::2].astype(BF16), total[0::2]
            bit *= 2
        if layer + 1 < layers:
            both = jnp.concatenate([keep.astype(BF16), send], axis=0)
            arrived = swap(both, "tp", bit)
            total = both.astype(F32) + arrived[::-1].astype(F32)
            old = pieces[bit][pre:].astype(F32)
            far = (old + total[1]).astype(BF16)
        else:
            arrived = swap(send, "tp", bit)
            total = keep.astype(F32) + arrived.astype(F32)
        own = (own.astype(F32) + total[0]).astype(BF16)
    floats = own.astype(F32)
    squares = jnp.sum(floats * floats, axis=1)
    squares = sum([swap(squares, "tp", k) for k in range(1, m)], squares)
    inv_rms = lax.rsqrt(squares / width + EPSILON)
    return (floats * inv_rms[:, None] * finishing_rms_gains[None, :]).astype(BF16)


def solution(mesh):
    def step(*args):
        run = jax.shard_map(
            on_device,
            mesh=mesh,
            in_specs=(
                P(("grp", "sp"), "tp"),
                P(None, "sp", "tp"),
                P(None, "sp", "tp"),
                P(None, None, "tp"),
                P(None, "tp", None, None),
                P(None, "tp", None, None),
                P(None, "tp"),
                P(("grp", "sp")),
                P(("grp", "sp"), "tp"),
                P(None, "tp", "sp"),
                P(),
                P("tp"),
            ),
            out_specs=P(("grp", "sp"), "tp"),
            check_vma=False,
        )
        jax.eval_shape(run, *args)
        return run(*args)

    return step
```
